256 devices in a mesh: sp: 64 (over z, y, core), tp: 4 (over x).
Axes of the slice: x: 4, y: 4, z: 8, core: 2. Of those that a mesh axis runs over, the one named last changes fastest.
Arguments:
- stream: bfloat16 [65536, 4096], P('sp', 'tp'), may hold values from -11 to 11
- norm_gain: bfloat16 [3, 4096], P(None, 'tp'), may hold values from 0.099609375 to 1.8984375
- pool_weight: bfloat16 [3, 4, 1024, 1024], P(None, 'tp', 'sp'), may hold values from -0.1875 to 0.1875
- pool_scale: bfloat16 [3, 4096], P(None, 'tp'), may hold values from 0.099609375 to 1.8984375
Outputs:
- mixed: bfloat16 [65536, 4096], P('sp', 'tp')
The draws below stay inside these ranges and needn't reach their ends.
All inputs are finite; a program needn't handle non-finite values.
Results may differ from the reference program's by a relative error of at most 0.015.
Values may be sent and summed in bfloat16 or wider, within the bound.
A program may use at most 64 MiB of HBM per device.

```python
import jax
import jax.numpy as jnp
from jax import lax

D = 4096
POOL_GROUPS = 4
LAYERS = 3
GC = 1024
TOKENS = 65536


def draw_stream(key, part):
    noise_key, perm_key, row_key = jax.random.split(key, 3)
    levels = 0.5 * 3.0 ** (jnp.arange(POOL_GROUPS, dtype=jnp.float32) / (POOL_GROUPS - 1))
    levels = jax.random.permutation(perm_key, levels)
    column_scale = jnp.repeat(levels, GC)
    base_vals = jax.random.truncated_normal(noise_key, -6.0, 6.0, (TOKENS, D), jnp.float32)
    return (base_vals * column_scale[None, :]).astype(jnp.bfloat16)


def shard_levels(key, extent, cuts, low, largest):
    gain = 1.0
    for dim, shards_of in cuts:
        draws = jax.random.uniform(jax.random.fold_in(jax.random.fold_in(key, 6), dim), (shards_of,), jnp.float32, low / len(cuts), largest / len(cuts))
        gain = gain * jnp.repeat(jnp.exp(draws), extent[dim] // shards_of).reshape((-1,) + (1,) * (len(extent) - 1 - dim))
    return gain


def noise(key, shape, scale, bound, cuts=(), kind=jnp.bfloat16):
    factor_of = shard_levels(key, shape, cuts, -0.22, 0.18) if cuts else 1.0
    drawn = jax.random.normal(key, shape, jnp.float32) * scale * factor_of
    return jnp.minimum(jnp.maximum(drawn, -bound), bound).astype(kind)


def setup_inputs(seed: int = 0) -> dict:
    splits = jax.random.split(jax.random.key(seed), 5)
    stream = draw_stream(jax.random.fold_in(splits[4], 71), 0)
    norm_gain = jnp.clip(1.0 + 0.18 * jax.random.normal(splits[1], (LAYERS, D), jnp.float32), 0.099609375, 1.8984375).astype(jnp.bfloat16)
    pool_weight = noise(splits[2], (LAYERS, POOL_GROUPS, GC, GC), GC ** -0.5, 0.1875, ((1, 4), (2, 64)))
    pool_scale = jnp.clip(1.0 + 0.18 * jax.random.normal(splits[3], (LAYERS, D), jnp.float32), 0.099609375, 1.8984375).astype(jnp.bfloat16)
    return {"stream": stream, "norm_gain": norm_gain, "pool_weight": pool_weight, "pool_scale": pool_scale}


norm_eps = 1e-06

def centred_mean(values, half_width):
    length = values.shape[0]
    sums = jnp.concatenate([jnp.zeros((1, values.shape[1]), jnp.float32), jnp.cumsum(values, axis=0)], axis=0)
    positions = jnp.arange(length)
    low_end = jnp.maximum(positions - half_width, 0)
    high_end = jnp.minimum(positions + half_width, length)
    return (sums[high_end] - sums[low_end]) / (high_end - low_end).astype(jnp.float32)[:, None]

def reference(stream, norm_gain, pool_weight, pool_scale):
    current = stream
    for layer_idx in range(LAYERS):
        stream_f = current.astype(jnp.float32)
        meansq = lax.optimization_barrier(jnp.mean(stream_f * stream_f, axis=1, keepdims=True))
        normed = (stream_f * lax.rsqrt(meansq + norm_eps) * norm_gain[layer_idx].astype(jnp.float32)).astype(jnp.bfloat16)
        pieces = []
        for group in range(POOL_GROUPS):
            members = normed[:, group * GC:(group + 1) * GC].astype(jnp.float32)
            pooled = (centred_mean(members, 2 ** group) - members).astype(jnp.bfloat16)
            pieces.append(jnp.dot(pooled, pool_weight[layer_idx, group], preferred_element_type=jnp.float32))
        branch = jnp.concatenate(pieces, axis=1)
        current = (stream_f + branch * pool_scale[layer_idx].astype(jnp.float32)).astype(jnp.bfloat16)
    return current
```

```python
import functools

import jax
import jax.numpy as jnp
from jax import lax
from jax.experimental import pallas as pl
from jax.experimental.pallas import tpu as pltpu
from jax.sharding import PartitionSpec as P

D = 4096
POOL_GROUPS = 4
NORM_EPS = 1e-06
PAD = 64
HALO = 32
TILE = 128
WINDOW = TILE + 2 * PAD
NY = 4
STAGGER = 3
ROUNDS = 6
ALONG_Z, ALONG_Y, ACROSS = 0, 1, 2
MESH = pl.DeviceIdType.MESH


def kernel(cfg, x_hbm, w_hbm, gain_hbm, scale_hbm, out_ref, gain_ref, scale_ref, xs, ps, ws, band, fac_in, fac, ss_own, ss_in,
           load_sem, halo_send, halo_recv, ss_send, ss_recv, w_send, w_recv, out_sem):
    layers, rows, width, shard_rows, n_sp, n_tp = cfg
    sp, tp = lax.axis_index("sp"), lax.axis_index("tp")
    nz = n_sp // (2 * NY)
    z, y, c = sp // (2 * NY), (sp // 2) % NY, sp % 2
    tiles = (rows + 2 * PAD) // TILE
    seq_total = rows * n_sp
    base_pos = sp * rows - PAD
    half = jnp.left_shift(jnp.int32(1), tp)
    has_prev, has_next = sp > 0, sp < n_sp - 1

    x_load = pltpu.make_async_copy(x_hbm, xs.at[pl.ds(2 * PAD, rows)], load_sem.at[layers])
    w_loads = [pltpu.make_async_copy(w_hbm.at[l, 0], ws.at[l, z, y, c], load_sem.at[l]) for l in range(layers)]
    gain_load = pltpu.make_async_copy(gain_hbm, gain_ref, load_sem.at[layers + 1])
    scale_load = pltpu.make_async_copy(scale_hbm, scale_ref, load_sem.at[layers + 2])
    w_loads[0].start()
    x_load.start()
    for l in range(1, layers):
        w_loads[l].start()
    gain_load.start()
    scale_load.start()

    def at_z(step):
        return ((lax.rem(z + step + nz, nz) * NY + y) * 2 + c, tp)

    def at_y(step):
        return ((z * NY + lax.rem(y + step + NY, NY)) * 2 + c, tp)

    partner = ((z * NY + y) * 2 + 1 - c, tp)

    barrier = pltpu.get_barrier_semaphore()

    def greet(device):
        pl.semaphore_signal(barrier, inc=1, device_id=device, device_id_type=MESH)

    for device in [at_z(1), at_z(-1), at_y(1), at_y(-1), at_y(2), partner]:
        greet(device)
    for p in range(1, n_tp):
        greet((sp, lax.rem(tp + p, n_tp)))
    pl.when(has_prev)(lambda: greet((sp - 1, tp)))
    pl.when(has_next)(lambda: greet((sp + 1, tp)))
    expected = 6 + n_tp - 1 + has_prev.astype(jnp.int32) + has_next.astype(jnp.int32)

    zero = jnp.zeros((2 * PAD, width), jnp.bfloat16)
    xs[pl.ds(0, 2 * PAD - HALO)] = zero[: 2 * PAD - HALO]
    xs[pl.ds(2 * PAD + rows + HALO, 2 * PAD - HALO)] = zero[: 2 * PAD - HALO]

    @pl.when(jnp.logical_not(has_prev))
    def _():
        xs[pl.ds(2 * PAD - HALO, HALO)] = zero[:HALO]

    @pl.when(jnp.logical_not(has_next))
    def _():
        xs[pl.ds(2 * PAD + rows, HALO)] = zero[:HALO]

    ss_own[...] = jnp.zeros(ss_own.shape, jnp.float32)
    fac_in[...] = jnp.zeros(fac_in.shape, jnp.float32)

    pl.semaphore_wait(barrier, expected)

    to_next = pltpu.make_async_remote_copy(
        x_hbm.at[pl.ds(rows - HALO, HALO)], xs.at[pl.ds(2 * PAD - HALO, HALO)],
        halo_send.at[0], halo_recv.at[0], device_id=(sp + 1, tp), device_id_type=MESH)
    to_prev = pltpu.make_async_remote_copy(
        x_hbm.at[pl.ds(0, HALO)], xs.at[pl.ds(2 * PAD + rows, HALO)],
        halo_send.at[1], halo_recv.at[1], device_id=(sp - 1, tp), device_id_type=MESH)

    def start_halo():
        pl.when(has_next)(lambda: to_next.start())
        pl.when(has_prev)(lambda: to_prev.start())

    def zz(step):
        return lax.rem(z + step + nz, nz)

    def yy(step):
        return lax.rem(y + step + NY, NY)

    def shard_copy(l, dz, dy, device, way):
        zs, ys = zz(dz), yy(dy)
        piece = ws.at[l, zs, ys, c]
        return pltpu.make_async_remote_copy(
            piece, piece, w_send.at[l, way], w_recv.at[l, (zs * NY + ys) * 2 + c],
            device_id=device, device_id_type=MESH)

    def z_out(l, dz, dy, step):
        shard_copy(l, dz, dy, at_z(step), ALONG_Z).start()

    def y_out(l, dz):
        for step in (1, -1, 2):
            shard_copy(l, dz, 0, at_y(step), ALONG_Y).start()

    def got(l, dz, dy):
        shard_copy(l, dz, dy, partner, ALONG_Z).wait_recv()

    def slab_copy(l, zs, core):
        slab = ws.at[l, zs, :, core]
        return pltpu.make_async_remote_copy(
            slab, slab, w_send.at[l, ACROSS], w_recv.at[l, zs * NY * 2 + core],
            device_id=partner, device_id_type=MESH)

    def across(l, dz):
        slab_copy(l, zz(dz), c).start()

    def got_across(l):
        for zs in range(nz):
            slab_copy(l, zs, 1 - c).wait_recv()

    far = nz // 2

    def z_first(l, k):
        if k == 0:
            z_out(l, 0, 0, 1)
            z_out(l, 0, 0, -1)
            y_out(l, 0)
        if 1 <= k <= far:
            got(l, -k, 0)
            if k < far:
                z_out(l, -k, 0, 1)
            if k < far:
                got(l, k, 0)
                if k < far - 1:
                    z_out(l, k, 0, -1)
            y_out(l, -k)
            if k < far:
                y_out(l, k)
        if k >= 1:
            j = k - 1
            for dz in ([0] if j == 0 else [-j] if j == far else [-j, j]):
                for dy in (1, -1, 2):
                    got(l, dz, dy)
                across(l, dz)

    def z_hop(l, k, dy):
        up_far = dy in (0, 3)
        if k < far or up_far:
            got(l, -k, dy)
            if k < far - 1 or (k == far - 1 and up_far):
                z_out(l, -k, dy, 1)
        if k < far or not up_far:
            got(l, k, dy)
            if k < far - 1 or (k == far - 1 and not up_far):
                z_out(l, k, dy, -1)

    def y_first(l, k):
        if k == 0:
            y_out(l, 0)
            z_out(l, 0, 0, 1)
            z_out(l, 0, 0, -1)
        if k == 1:
            for dy in (1, 3):
                got(l, 0, dy)
                z_out(l, 0, dy, 1)
                z_out(l, 0, dy, -1)
            z_hop(l, 1, 0)
            got(l, 0, 2)
            z_out(l, 0, 2, 1)
            z_out(l, 0, 2, -1)
            across(l, 0)
        if k >= 2:
            if k <= far:
                z_hop(l, k, 0)
            for dy in (1, 3, 2):
                z_hop(l, k - 1, dy)
            j = k - 1
            for dz in ([-j] if j == far else [-j, j]):
                across(l, dz)

    def comm_round(l, k):
        if k == 0:
            w_loads[l].wait()
        pl.when(c == 0)(lambda: z_first(l, k))
        pl.when(c == 1)(lambda: y_first(l, k))

    def build_band():
        @pl.loop(0, tiles)
        def _(i):
            offset = (
                lax.broadcasted_iota(jnp.int32, (TILE, WINDOW), 1)
                - lax.broadcasted_iota(jnp.int32, (TILE, WINDOW), 0)
                - PAD
            )
            pos = base_pos + i * TILE + lax.broadcasted_iota(jnp.int32, (TILE, WINDOW), 0)
            count = jnp.minimum(pos + half, seq_total) - jnp.maximum(pos - half, 0)
            inverse = 1.0 / jnp.maximum(count, 1).astype(jnp.float32)
            mean = jnp.where((offset >= -half) & (offset < half), inverse, 0.0)
            band[i] = mean - jnp.where(offset == 0, 1.0, 0.0)

    def store_sums(layer, i, part):
        ss_own[layer, pl.ds(i, 1)] = jnp.sum(part.T, axis=0, keepdims=True)

    def square_sums():
        @pl.loop(0, tiles // 3)
        def _(b):
            for t in range(3):
                i = b * 3 + t
                part = jnp.zeros((TILE, 128), jnp.float32)
                for n in range(width // 128):
                    v = xs[pl.ds(pl.multiple_of(PAD + i * TILE, 64), TILE), pl.ds(n * 128, 128)].astype(jnp.float32)
                    part = part + v * v
                store_sums(0, i, part)

    def ss_copy(layer, p):
        return pltpu.make_async_remote_copy(
            ss_own.at[layer], ss_in.at[layer, p - 1], ss_send.at[layer, p - 1], ss_recv.at[layer, p - 1],
            device_id=(sp, lax.rem(tp + p, n_tp)), device_id_type=MESH)

    def send_sums(layer):
        for p in range(1, n_tp):
            ss_copy(layer, p).start()

    def factors(layer):
        for p in range(1, n_tp):
            ss_copy(layer, p).wait()
        total = ss_own[layer]
        for p in range(1, n_tp):
            total = total + ss_in[layer, p - 1]
        factor = lax.rsqrt(total / D + NORM_EPS)
        tile = lax.broadcasted_iota(jnp.int32, total.shape, 0)
        lane = lax.broadcasted_iota(jnp.int32, total.shape, 1)
        pos = base_pos + tile * TILE + lane
        factor = jnp.where((pos >= 0) & (pos < seq_total) & (tile < tiles), factor, 0.0)
        fac_in[pl.ds(8, 16)] = factor
        low = pltpu.roll(fac_in[pl.ds(7, 16)], PAD, 1)
        high = pltpu.roll(factor, PAD, 1)
        fac[...] = jnp.where(lane < PAD, low, high)

    def pool(layer, b):
        for t in range(3):
            i = b * 3 + t
            factor = jnp.concatenate([fac[i : i + 1], fac[i + 1 : i + 2]], axis=1)
            weights = (band[i] * factor).astype(jnp.bfloat16)
            for n in range(width // 256):
                cols = pl.ds(n * 256, 256)
                sums = jnp.dot(weights, xs[pl.ds(i * TILE, WINDOW), cols], preferred_element_type=jnp.float32)
                g = gain_ref[layer : layer + 1, cols].astype(jnp.float32)
                ps[pl.ds(i * TILE, TILE), cols] = (sums * g).astype(jnp.bfloat16)

    def mixed_block(layer, first_row, block, n):
        cols = pl.ds(n * 256, 256)
        weight = ws[layer, :, :, :, :, cols].reshape(width, 256)
        branch = jnp.dot(ps[pl.ds(first_row, block)], weight, preferred_element_type=jnp.float32)
        s = scale_ref[layer : layer + 1, cols].astype(jnp.float32)
        at = pl.ds(PAD + first_row, block)
        mixed = (xs[at, cols].astype(jnp.float32) + branch * s).astype(jnp.bfloat16)
        xs[at, cols] = mixed
        return mixed

    def mix(layer, b):
        block = 3 * TILE
        part = jnp.zeros((block, 128), jnp.float32)
        for n in range(width // 256):
            v = mixed_block(layer, b * block, block, n).astype(jnp.float32)
            sq = v * v
            part = part + sq[:, :128] + sq[:, 128:]
        for t in range(3):
            store_sums(layer + 1, b * 3 + t, part[t * TILE : (t + 1) * TILE])

    def start_work():
        x_load.wait()
        gain_load.wait()
        scale_load.wait()
        pl.when(has_prev)(lambda: to_next.wait_recv())
        pl.when(has_next)(lambda: to_prev.wait_recv())

    tasks = {}

    def do(t, *work):
        tasks.setdefault(t, []).extend(work)

    part = functools.partial
    do(0, start_halo, build_band)
    do(1, start_work, square_sums, part(send_sums, 0))
    do(2, part(factors, 0), part(pool, 0, 0))
    do(3, part(pool, 0, 1), part(pool, 0, 2))
    for layer in range(layers - 1):
        t = ROUNDS - 1 + STAGGER * layer
        do(t, part(got_across, layer), part(mix, layer, 0))
        do(t + 1, part(mix, layer, 1))
        do(t + 2, part(mix, layer, 2), part(send_sums, layer + 1))
        do(t + 3, part(factors, layer + 1), part(pool, layer + 1, 0), part(pool, layer + 1, 1), part(pool, layer + 1, 2))

    last = layers - 1
    for t in range(ROUNDS + STAGGER * last):
        for l in range(layers):
            if 0 <= t - STAGGER * l < ROUNDS:
                comm_round(l, t - STAGGER * l)
        for work in tasks.get(t, []):
            work()
    got_across(last)

    outs = []
    block = rows // 2
    for b in range(2):
        for n in range(width // 256):
            mixed_block(last, PAD + b * block, block, n)
            at, cols = pl.ds(2 * PAD + b * block, block), pl.ds(n * 256, 256)
            outs.append(pltpu.make_async_copy(
                xs.at[at, cols], out_ref.at[pl.ds(b * block, block), cols], out_sem.at[len(outs)]))
            outs[-1].start()

    pl.when(has_next)(lambda: to_next.wait_send())
    pl.when(has_prev)(lambda: to_prev.wait_send())

    def drain(l, way, refs):
        pltpu.make_async_remote_copy(
            refs, refs, w_send.at[l, way], w_recv.at[l, 0], device_id=partner, device_id_type=MESH).wait_send()

    for l in range(layers):
        drain(l, ACROSS, ws.at[l, :, :, 0])

        @pl.when(c == 0)
        def _():
            drain(l, ALONG_Z, ws.at[l, pl.ds(0, nz - 1), 0, 0])
            drain(l, ALONG_Y, ws.at[l, :, pl.ds(0, NY - 1), 0])

        @pl.when(c == 1)
        def _():
            drain(l, ALONG_Z, ws.at[l, pl.ds(0, nz - 1), :, 0])
            drain(l, ALONG_Y, ws.at[l, 0, pl.ds(0, NY - 1), 0])

    for out in outs:
        out.wait()


def solution(mesh):
    n_sp, n_tp = mesh.shape["sp"], mesh.shape["tp"]

    def local(stream, norm_gain, pool_weight, pool_scale):
        rows, _ = stream.shape
        layers, per_dev, shard_rows, width = pool_weight.shape
        assert per_dev == 1 and n_tp == POOL_GROUPS and n_sp % (4 * NY) == 0
        total_rows = rows + 2 * PAD
        dma = pltpu.SemaphoreType.DMA
        hbm = pl.BlockSpec(memory_space=pltpu.HBM)
        return pl.pallas_call(
            functools.partial(kernel, (layers, rows, width, shard_rows, n_sp, n_tp)),
            out_shape=jax.ShapeDtypeStruct((rows, width), jnp.bfloat16),
            in_specs=[hbm] * 4,
            out_specs=hbm,
            scratch_shapes=[
                pltpu.VMEM((layers, width), jnp.bfloat16),
                pltpu.VMEM((layers, width), jnp.bfloat16),
                pltpu.VMEM((total_rows + 2 * PAD, width), jnp.bfloat16),
                pltpu.VMEM((total_rows, width), jnp.bfloat16),
                pltpu.VMEM((layers, n_sp // (2 * NY), NY, 2, shard_rows, width), jnp.bfloat16),
                pltpu.VMEM((total_rows // TILE, TILE, WINDOW), jnp.float32),
                pltpu.VMEM((24, TILE), jnp.float32),
                pltpu.VMEM((16, TILE), jnp.float32),
                pltpu.VMEM((layers, 16, TILE), jnp.float32),
                pltpu.VMEM((layers, n_tp - 1, 16, TILE), jnp.float32),
                dma((layers + 3,)),
                dma((2,)),
                dma((2,)),
                dma((layers, n_tp - 1)),
                dma((layers, n_tp - 1)),
                dma((layers, 3)),
                dma((layers, n_sp)),
                dma((8,)),
            ],
            compiler_params=pltpu.CompilerParams(
                collective_id=0, has_side_effects=True, vmem_limit_bytes=60 * 2**20
            ),
        )(stream, pool_weight, norm_gain, pool_scale)

    placed = (P("sp", "tp"), P(None, "tp"), P(None, "tp", "sp", None), P(None, "tp"))
    return jax.shard_map(
        local, mesh=mesh, in_specs=placed, out_specs=P("sp", "tp"), check_vma=False
    )
```

```python
import functools

import jax
import jax.numpy as jnp
from jax import lax
from jax.experimental import pallas as pl
from jax.experimental.pallas import tpu as pltpu
from jax.sharding import PartitionSpec as P

D = 4096
POOL_GROUPS = 4
NORM_EPS = 1e-06
PAD = 64
HALO = 32
TILE = 128
WINDOW = TILE + 2 * PAD
PER = 3
BLOCKS = 3
NY = 4
FAST = (False, False, False)
PLAN = (
    ((30, 130, 20, 40, 31, 33), (30, 130, 20, 40, 33, 31), 'x00'),
    ((32, 120, 140, 131, 133, 230, 10, 21, 23, 132, 50, 43, 41, 22), (32, 120, 133, 131, 10, 50, 140, 230, 43, 23, 21, 41, 132, 22, 42, 143), 'q00'),
    ((42, 110, 150, 121, 123, 141, 143), (110, 123, 141, 60, 121), 'q01'),
    ((122, 231, 233), (0, 150, 231, 233, 220, 240), 'q02'),
    ((142, 220, 11, 13, 240, 232, 0, 53, 51, 60, 12, 113, 111, 52, 100, 153, 151, 160, 112, 223, 221, 152, 243, 241, 3, 1, 222, 210, 250, 242, 63, 61, 2, 70, 103, 101, 62, 163, 161, 102, 213, 211, 170, 162, 253, 251, 212, 260, 71, 73, 252, 200, 72), (13, 51, 53, 232, 11, 142, 122, 12, 52, 100, 153, 151, 113, 111, 160, 70, 241, 221, 243, 223, 250, 210, 61, 63, 3, 222, 242, 1, 152, 62, 112, 163, 2, 161, 170, 251, 103, 253, 260, 101, 71, 211, 252, 213, 200, 162, 73, 72, 171, 212, 261, 102, 263, 173, 262, 201, 172, 203), 'm00'),
    ((171, 173), (270, 202, 271), 'm01'),
    ((172, 261, 263), (273, 272), 'm02'),
    ((270, 201, 203, 262, 202, 273, 271), (), 'q10'),
    ((), (), 'm10'),
    ((272,), (), 'q11'),
    ((), (), 'm11'),
    ((), (), 'q12'),
    ((), (), 'm12'),
    ((), (), 'q20'),
    ((), (), 'm20'),
    ((), (), 'q21'),
    ((), (), 'm21'),
    ((), (), 'q22'),
    ((), (), 'm22'),
    ((), (), ''),
)
ALONG_Z, ALONG_Y, ACROSS = 0, 1, 2
MESH = pl.DeviceIdType.MESH


def kernel(cfg, x_hbm, w_hbm, gain_hbm, scale_hbm, out_ref, gain_ref, scale_ref, xs, ps, ws, band, fac, ss_own, ss_in,
           load_sem, halo_send, halo_recv, ss_send, ss_recv, w_send, w_recv):
    layers, rows, width, shard_rows, n_sp, n_tp = cfg
    sp, tp = lax.axis_index("sp"), lax.axis_index("tp")
    nz = n_sp // (2 * NY)
    z, y, c = sp // (2 * NY), (sp // 2) % NY, sp % 2
    tiles = (rows + 2 * PAD) // TILE
    seq_total = rows * n_sp
    base_pos = sp * rows - PAD
    half = jnp.left_shift(jnp.int32(1), tp)
    has_prev, has_next = sp > 0, sp < n_sp - 1

    x_load = pltpu.make_async_copy(x_hbm, xs.at[0, pl.ds(2 * PAD, rows)], load_sem.at[layers])
    w_loads = [pltpu.make_async_copy(w_hbm.at[l, 0], ws.at[l, z, y, c], load_sem.at[l]) for l in range(layers)]
    gain_load = pltpu.make_async_copy(gain_hbm, gain_ref, load_sem.at[layers + 1])
    scale_load = pltpu.make_async_copy(scale_hbm, scale_ref, load_sem.at[layers + 2])
    w_loads[0].start()
    x_load.start()
    for l in range(1, layers):
        w_loads[l].start()
    gain_load.start()
    scale_load.start()

    def at_z(step):
        return ((lax.rem(z + step + nz, nz) * NY + y) * 2 + c, tp)

    def at_y(step):
        return ((z * NY + lax.rem(y + step + NY, NY)) * 2 + c, tp)

    partner = ((z * NY + y) * 2 + 1 - c, tp)

    barrier = pltpu.get_barrier_semaphore()

    def greet(device):
        pl.semaphore_signal(barrier, inc=1, device_id=device, device_id_type=MESH)

    for device in [at_z(1), at_z(-1), at_y(1), at_y(-1), at_y(2), partner]:
        greet(device)
    for p in range(1, n_tp):
        greet((sp, lax.rem(tp + p, n_tp)))
    pl.when(has_prev)(lambda: greet((sp - 1, tp)))
    pl.when(has_next)(lambda: greet((sp + 1, tp)))
    expected = 6 + n_tp - 1 + has_prev.astype(jnp.int32) + has_next.astype(jnp.int32)

    zero = jnp.zeros((2 * PAD, width), jnp.bfloat16)
    xs[0, pl.ds(0, 2 * PAD - HALO)] = zero[: 2 * PAD - HALO]
    xs[0, pl.ds(2 * PAD + rows + HALO, 2 * PAD - HALO)] = zero[: 2 * PAD - HALO]
    xs[1, pl.ds(0, PAD)] = zero[:PAD]
    xs[1, pl.ds(3 * PAD + rows, PAD)] = zero[:PAD]

    @pl.when(jnp.logical_not(has_prev))
    def _():
        xs[0, pl.ds(2 * PAD - HALO, HALO)] = zero[:HALO]

    @pl.when(jnp.logical_not(has_next))
    def _():
        xs[0, pl.ds(2 * PAD + rows, HALO)] = zero[:HALO]

    ss_own[...] = jnp.zeros(ss_own.shape, jnp.float32)
    fac[...] = jnp.zeros(fac.shape, jnp.float32)

    pl.semaphore_wait(barrier, expected)

    to_next = pltpu.make_async_remote_copy(
        x_hbm.at[pl.ds(rows - HALO, HALO)], xs.at[0, pl.ds(2 * PAD - HALO, HALO)],
        halo_send.at[0], halo_recv.at[0], device_id=(sp + 1, tp), device_id_type=MESH)
    to_prev = pltpu.make_async_remote_copy(
        x_hbm.at[pl.ds(0, HALO)], xs.at[0, pl.ds(2 * PAD + rows, HALO)],
        halo_send.at[1], halo_recv.at[1], device_id=(sp - 1, tp), device_id_type=MESH)

    def start_halo():
        pl.when(has_next)(lambda: to_next.start())
        pl.when(has_prev)(lambda: to_prev.start())

    def zz(step):
        return lax.rem(z + step + nz, nz)

    def yy(step):
        return lax.rem(y + step + NY, NY)

    def shard_copy(l, dz, dy, device, way):
        zs, ys = zz(dz), yy(dy)
        piece = ws.at[l, zs, ys, c]
        return pltpu.make_async_remote_copy(
            piece, piece, w_send.at[l, way], w_recv.at[l, (zs * NY + ys) * 2 + c],
            device_id=device, device_id_type=MESH)

    def z_out(l, dz, dy, step):
        shard_copy(l, dz, dy, at_z(step), ALONG_Z).start()

    def y_out(l, dz):
        for step in (1, -1, 2):
            shard_copy(l, dz, 0, at_y(step), ALONG_Y).start()

    def got(l, dz, dy):
        shard_copy(l, dz, dy, partner, ALONG_Z).wait_recv()

    def slab_copy(l, zs, core):
        slab = ws.at[l, zs, :, core]
        return pltpu.make_async_remote_copy(
            slab, slab, w_send.at[l, ACROSS], w_recv.at[l, zs * NY * 2 + core],
            device_id=partner, device_id_type=MESH)

    def across(l, dz):
        slab_copy(l, zz(dz), c).start()

    def got_across(l):
        for zs in range(nz):
            slab_copy(l, zs, 1 - c).wait_recv()

    far = nz // 2

    def goes_up(dy):
        return dy in (0, 3)

    def z_steps(l, dz, dy, up):
        if FAST[l]:
            return {0: (2, -2, 1, -1), -2: (2, 1) if up else (1,), 2: (-1,) if up else (-2, -1)}.get(dz, ())
        if dz == 0:
            return (1, -1)
        if dz < 0:
            return (1,) if -dz < far - 1 + up else ()
        return (-1,) if dz < far - up else ()

    seen = {}

    def pass_on(core, event):
        l, dz, dy = event // 100, event // 10 % 10 - 3, event % 10
        if (dz, dy) == (0, 0):
            w_loads[l].wait()
        else:
            got(l, dz, dy)
        if core == 0:
            if dy == 0:
                for step in z_steps(l, dz, dy, 1):
                    z_out(l, dz, dy, step)
                y_out(l, dz)
        else:
            if (dz, dy) == (0, 0):
                y_out(l, dz)
            for step in z_steps(l, dz, dy, int(goes_up(dy))):
                z_out(l, dz, dy, step)
        seen[core, l, dz] = seen.get((core, l, dz), 0) + 1
        if seen[core, l, dz] == NY:
            across(l, dz)

    def pass_all(core, events):
        for event in events:
            pass_on(core, event)

    def build_band():
        @pl.loop(0, tiles)
        def _(i):
            offset = (
                lax.broadcasted_iota(jnp.int32, (TILE, WINDOW), 1)
                - lax.broadcasted_iota(jnp.int32, (TILE, WINDOW), 0)
                - PAD
            )
            pos = base_pos + i * TILE + lax.broadcasted_iota(jnp.int32, (TILE, WINDOW), 0)
            count = jnp.minimum(pos + half, seq_total) - jnp.maximum(pos - half, 0)
            inverse = 1.0 / jnp.maximum(count, 1).astype(jnp.float32)
            mean = jnp.where((offset >= -half) & (offset < half), inverse, 0.0)
            band[i] = mean - jnp.where(offset == 0, 1.0, 0.0)

    def store_sums(layer, b, t, part):
        ss_own[layer, b, pl.ds(t, 1)] = jnp.sum(part.T, axis=0, keepdims=True)

    def square_sums():
        @pl.loop(0, BLOCKS)
        def _(b):
            for t in range(PER):
                row = pl.multiple_of(PAD + b * (PER * TILE), 64) + t * TILE
                part = jnp.zeros((TILE, 128), jnp.float32)
                for n in range(width // 128):
                    v = xs[0, pl.ds(row, TILE), pl.ds(n * 128, 128)].astype(jnp.float32)
                    part = part + v * v
                store_sums(0, b, t, part)

    def ss_copy(layer, b, p):
        return pltpu.make_async_remote_copy(
            ss_own.at[layer, b], ss_in.at[layer, p - 1, b], ss_send.at[layer, p - 1, b], ss_recv.at[layer, p - 1, b],
            device_id=(sp, lax.rem(tp + p, n_tp)), device_id_type=MESH)

    def send_sums(layer, b):
        for p in range(1, n_tp):
            ss_copy(layer, b, p).start()

    def factors(layer, b):
        for p in range(1, n_tp):
            ss_copy(layer, b, p).wait()
        total = ss_own[layer, b]
        for p in range(1, n_tp):
            total = total + ss_in[layer, p - 1, b]
        factor = lax.rsqrt(total / D + NORM_EPS)
        tile = b * PER + lax.broadcasted_iota(jnp.int32, total.shape, 0)
        pos = base_pos + tile * TILE + lax.broadcasted_iota(jnp.int32, total.shape, 1)
        factor = jnp.where((pos >= 0) & (pos < seq_total), factor, 0.0)
        fac[pl.ds(8 + b * PER, PER)] = factor[:PER]

    def pool(layer, b):
        low = pltpu.roll(fac[pl.ds(7 + b * PER, PER + 1)], PAD, 1)
        high = pltpu.roll(fac[pl.ds(8 + b * PER, PER + 1)], PAD, 1)
        lane = lax.broadcasted_iota(jnp.int32, low.shape, 1)
        shifted = jnp.where(lane < PAD, low, high)
        for t in range(PER):
            i = b * PER + t
            factor = jnp.concatenate([shifted[t : t + 1], shifted[t + 1 : t + 2]], axis=1)
            weights = (band[i] * factor).astype(jnp.bfloat16)
            for n in range(width // 256):
                cols = pl.ds(n * 256, 256)
                window = xs[layer % 2, pl.ds(i * TILE, WINDOW), cols]
                sums = jnp.dot(weights, window, preferred_element_type=jnp.float32)
                g = gain_ref[layer : layer + 1, cols].astype(jnp.float32)
                ps[pl.ds(i * TILE, TILE), cols] = (sums * g).astype(jnp.bfloat16)

    def mixed_block(layer, first_row, block, n):
        cols = pl.ds(n * 256, 256)
        weight = ws[layer, :, :, :, :, cols].reshape(width, 256)
        branch = jnp.dot(ps[pl.ds(first_row, block)], weight, preferred_element_type=jnp.float32)
        s = scale_ref[layer : layer + 1, cols].astype(jnp.float32)
        old = xs[layer % 2, pl.ds(PAD + first_row, block), cols].astype(jnp.float32)
        return (old + branch * s).astype(jnp.bfloat16)

    def mix(layer, b):
        block = PER * TILE
        part = jnp.zeros((block, 128), jnp.float32)
        for n in range(width // 256):
            mixed = mixed_block(layer, b * block, block, n)
            xs[(layer + 1) % 2, pl.ds(PAD + b * block, block), pl.ds(n * 256, 256)] = mixed
            v = mixed.astype(jnp.float32)
            sq = v * v
            part = part + sq[:, :128] + sq[:, 128:]
        for t in range(PER):
            store_sums(layer + 1, b, t, part[t * TILE : (t + 1) * TILE])
        send_sums(layer + 1, b)

    def mix_out(layer, b):
        first = max(b * PER * TILE, PAD)
        block = min((b + 1) * PER * TILE, PAD + rows) - first
        for n in range(width // 256):
            out_ref[pl.ds(first - PAD, block), pl.ds(n * 256, 256)] = mixed_block(layer, first, block, n)

    def start_work():
        x_load.wait()
        gain_load.wait()
        scale_load.wait()
        pl.when(has_prev)(lambda: to_next.wait_recv())
        pl.when(has_next)(lambda: to_prev.wait_recv())

    last = layers - 1

    def task(name):
        kind, l, b = name[0], int(name[1]), int(name[2])
        if kind == "x":
            start_work()
            square_sums()
            for block in range(BLOCKS):
                send_sums(0, block)
        elif kind == "q":
            if b == 0:
                factors(l, 0)
            if b < BLOCKS - 1:
                factors(l, b + 1)
            pool(l, b)
        elif kind == "m":
            if b == 0:
                got_across(l)
            (mix_out if l == last else mix)(l, b)

    for l in range(layers):
        if l * 100 + 30 in PLAN[0][0]:
            pl.when(c == 0)(functools.partial(pass_on, 0, l * 100 + 30))
            pl.when(c == 1)(functools.partial(pass_on, 1, l * 100 + 30))
    start_halo()
    build_band()
    for first, second, name in PLAN:
        if name == "x00":
            first = [e for e in first if e % 100 != 30]
            second = [e for e in second if e % 100 != 30]
        if first:
            pl.when(c == 0)(functools.partial(pass_all, 0, first))
        if second:
            pl.when(c == 1)(functools.partial(pass_all, 1, second))
        if name:
            task(name)
    pl.when(has_next)(lambda: to_next.wait_send())
    pl.when(has_prev)(lambda: to_prev.wait_send())

    def drain(l, way, refs):
        pltpu.make_async_remote_copy(
            refs, refs, w_send.at[l, way], w_recv.at[l, 0], device_id=partner, device_id_type=MESH).wait_send()

    for l in range(layers):
        drain(l, ACROSS, ws.at[l, :, :, 0])

        @pl.when(c == 0)
        def _():
            drain(l, ALONG_Z, ws.at[l, pl.ds(0, nz - 1), 0, 0])
            drain(l, ALONG_Y, ws.at[l, :, pl.ds(0, NY - 1), 0])

        @pl.when(c == 1)
        def _():
            drain(l, ALONG_Z, ws.at[l, pl.ds(0, nz - 1), :, 0])
            drain(l, ALONG_Y, ws.at[l, 0, pl.ds(0, NY - 1), 0])


def solution(mesh):
    n_sp, n_tp = mesh.shape["sp"], mesh.shape["tp"]

    def local(stream, norm_gain, pool_weight, pool_scale):
        rows, _ = stream.shape
        layers, per_dev, shard_rows, width = pool_weight.shape
        assert per_dev == 1 and n_tp == POOL_GROUPS and n_sp % (4 * NY) == 0
        total_rows = rows + 2 * PAD
        dma = pltpu.SemaphoreType.DMA
        hbm = pl.BlockSpec(memory_space=pltpu.HBM)
        return pl.pallas_call(
            functools.partial(kernel, (layers, rows, width, shard_rows, n_sp, n_tp)),
            out_shape=pltpu.VMEM((rows, width), jnp.bfloat16),
            in_specs=[hbm] * 4,
            out_specs=pl.BlockSpec(memory_space=pltpu.VMEM),
            scratch_shapes=[
                pltpu.VMEM((layers, width), jnp.bfloat16),
                pltpu.VMEM((layers, width), jnp.bfloat16),
                pltpu.VMEM((2, total_rows + 2 * PAD, width), jnp.bfloat16),
                pltpu.VMEM((total_rows, width), jnp.bfloat16),
                pltpu.VMEM((layers, n_sp // (2 * NY), NY, 2, shard_rows, width), jnp.bfloat16),
                pltpu.VMEM((total_rows // TILE, TILE, WINDOW), jnp.float32),
                pltpu.VMEM((24, TILE), jnp.float32),
                pltpu.VMEM((layers, BLOCKS, 8, TILE), jnp.float32),
                pltpu.VMEM((layers, n_tp - 1, BLOCKS, 8, TILE), jnp.float32),
                dma((layers + 3,)),
                dma((2,)),
                dma((2,)),
                dma((layers, n_tp - 1, BLOCKS)),
                dma((layers, n_tp - 1, BLOCKS)),
                dma((layers, 3)),
                dma((layers, n_sp)),
            ],
            compiler_params=pltpu.CompilerParams(
                collective_id=0, has_side_effects=True, vmem_limit_bytes=60 * 2**20
            ),
        )(stream, pool_weight, norm_gain, pool_scale)

    placed = (P("sp", "tp"), P(None, "tp"), P(None, "tp", "sp", None), P(None, "tp"))
    return jax.shard_map(
        local, mesh=mesh, in_specs=placed, out_specs=P("sp", "tp"), check_vma=False
    )
```

```python
import functools

import jax
import jax.numpy as jnp
from jax import lax
from jax.experimental import pallas as pl
from jax.experimental.pallas import tpu as pltpu
from jax.sharding import PartitionSpec as P

D = 4096
POOL_GROUPS = 4
NORM_EPS = 1e-06
PAD = 64
HALO = 32
TILE = 128
WINDOW = TILE + 2 * PAD
PER = 3
BLOCKS = 3
NY = 4
FAST = (False, False, False)
PLAN = (
    ((30,), (30,), 'b00'),
    ((20, 40, 31, 33, 130), (20, 40, 33, 31, 130), 'x00'),
    ((32, 23, 21, 10, 43, 41, 50, 230, 22, 120, 140, 131, 133), (32, 10, 50, 43, 23, 21, 41, 230, 131, 133, 120, 22, 42, 140), 'q00'),
    ((42, 132), (0, 13, 53, 60, 132, 51), 'q01'),
    ((13, 11), (11,), 'q02'),
    ((0, 60, 51, 53, 220, 240, 12, 231, 233, 52, 110, 232, 123, 121, 150, 143, 141, 122, 142, 3, 1, 70, 61, 63, 250, 223, 221, 2, 210, 243, 241, 62, 222, 113, 111, 242, 100, 160, 153, 151, 112, 73, 71, 152, 253, 251, 260, 213, 211, 72, 200, 252, 103, 101, 212, 163, 161), (220, 240, 121, 141, 231, 233, 143, 123, 110, 52, 232, 12, 150, 70, 63, 3, 142, 122, 61, 1, 250, 210, 151, 241, 111, 243, 221, 153, 223, 62, 113, 242, 100, 160, 222, 152, 2, 71, 73, 260, 112, 161, 200, 101, 251, 253, 211, 163, 213, 72, 103, 252), 'm00'),
    ((170, 102, 162, 201, 203, 261, 263), (162, 170, 102, 171, 212, 261, 263, 270), 'm01'),
    ((270, 202, 262), (203, 262, 201, 173), 'm02'),
    ((171, 173, 172, 273, 271), (172, 202, 271, 273, 272), 'q10'),
    ((), (), 'm10'),
    ((272,), (), 'q11'),
    ((), (), 'm11'),
    ((), (), 'q12'),
    ((), (), 'm12'),
    ((), (), 'q20'),
    ((), (), 'm20'),
    ((), (), 'q21'),
    ((), (), 'm21'),
    ((), (), 'q22'),
    ((), (), 'm22'),
    ((), (), ''),
)
ALONG_Z, ALONG_Y, ACROSS = 0, 1, 2
MESH = pl.DeviceIdType.MESH


def kernel(cfg, x_hbm, w_hbm, gain_hbm, scale_hbm, out_ref, gain_ref, scale_ref, xs, ps, ws, band, fac, ss_own, ss_in,
           load_sem, halo_send, halo_recv, ss_send, ss_recv, w_send, w_recv):
    layers, rows, width, shard_rows, n_sp, n_tp = cfg
    sp, tp = lax.axis_index("sp"), lax.axis_index("tp")
    nz = n_sp // (2 * NY)
    z, y, c = sp // (2 * NY), (sp // 2) % NY, sp % 2
    tiles = (rows + 2 * PAD) // TILE
    seq_total = rows * n_sp
    base_pos = sp * rows - PAD
    half = jnp.left_shift(jnp.int32(1), tp)
    has_prev, has_next = sp > 0, sp < n_sp - 1

    x_load = pltpu.make_async_copy(x_hbm, xs.at[0, pl.ds(2 * PAD, rows)], load_sem.at[layers])
    w_loads = [pltpu.make_async_copy(w_hbm.at[l, 0], ws.at[l, z, y, c], load_sem.at[l]) for l in range(layers)]
    gain_load = pltpu.make_async_copy(gain_hbm, gain_ref, load_sem.at[layers + 1])
    scale_load = pltpu.make_async_copy(scale_hbm, scale_ref, load_sem.at[layers + 2])
    w_loads[0].start()
    x_load.start()
    for l in range(1, layers):
        w_loads[l].start()
    gain_load.start()
    scale_load.start()

    def at_z(step):
        return ((lax.rem(z + step + nz, nz) * NY + y) * 2 + c, tp)

    def at_y(step):
        return ((z * NY + lax.rem(y + step + NY, NY)) * 2 + c, tp)

    partner = ((z * NY + y) * 2 + 1 - c, tp)

    barrier = pltpu.get_barrier_semaphore()

    def greet(device):
        pl.semaphore_signal(barrier, inc=1, device_id=device, device_id_type=MESH)

    for device in [at_z(1), at_z(-1), at_y(1), at_y(-1), at_y(2), partner]:
        greet(device)
    for p in range(1, n_tp):
        greet((sp, lax.rem(tp + p, n_tp)))
    pl.when(has_prev)(lambda: greet((sp - 1, tp)))
    pl.when(has_next)(lambda: greet((sp + 1, tp)))
    expected = 6 + n_tp - 1 + has_prev.astype(jnp.int32) + has_next.astype(jnp.int32)

    zero = jnp.zeros((2 * PAD, width), jnp.bfloat16)
    xs[0, pl.ds(0, 2 * PAD - HALO)] = zero[: 2 * PAD - HALO]
    xs[0, pl.ds(2 * PAD + rows + HALO, 2 * PAD - HALO)] = zero[: 2 * PAD - HALO]
    xs[1, pl.ds(0, PAD)] = zero[:PAD]
    xs[1, pl.ds(3 * PAD + rows, PAD)] = zero[:PAD]

    @pl.when(jnp.logical_not(has_prev))
    def _():
        xs[0, pl.ds(2 * PAD - HALO, HALO)] = zero[:HALO]

    @pl.when(jnp.logical_not(has_next))
    def _():
        xs[0, pl.ds(2 * PAD + rows, HALO)] = zero[:HALO]

    ss_own[...] = jnp.zeros(ss_own.shape, jnp.float32)
    fac[...] = jnp.zeros(fac.shape, jnp.float32)

    pl.semaphore_wait(barrier, expected)

    to_next = pltpu.make_async_remote_copy(
        x_hbm.at[pl.ds(rows - HALO, HALO)], xs.at[0, pl.ds(2 * PAD - HALO, HALO)],
        halo_send.at[0], halo_recv.at[0], device_id=(sp + 1, tp), device_id_type=MESH)
    to_prev = pltpu.make_async_remote_copy(
        x_hbm.at[pl.ds(0, HALO)], xs.at[0, pl.ds(2 * PAD + rows, HALO)],
        halo_send.at[1], halo_recv.at[1], device_id=(sp - 1, tp), device_id_type=MESH)

    def start_halo():
        pl.when(has_next)(lambda: to_next.start())
        pl.when(has_prev)(lambda: to_prev.start())

    def zz(step):
        return lax.rem(z + step + nz, nz)

    def yy(step):
        return lax.rem(y + step + NY, NY)

    def shard_copy(l, dz, dy, device, way):
        zs, ys = zz(dz), yy(dy)
        piece = ws.at[l, zs, ys, c]
        return pltpu.make_async_remote_copy(
            piece, piece, w_send.at[l, way], w_recv.at[l, (zs * NY + ys) * 2 + c],
            device_id=device, device_id_type=MESH)

    def z_out(l, dz, dy, step):
        shard_copy(l, dz, dy, at_z(step), ALONG_Z).start()

    def y_out(l, dz):
        for step in (1, -1, 2):
            shard_copy(l, dz, 0, at_y(step), ALONG_Y).start()

    def got(l, dz, dy):
        shard_copy(l, dz, dy, partner, ALONG_Z).wait_recv()

    def slab_copy(l, zs, core):
        slab = ws.at[l, zs, :, core]
        return pltpu.make_async_remote_copy(
            slab, slab, w_send.at[l, ACROSS], w_recv.at[l, zs * NY * 2 + core],
            device_id=partner, device_id_type=MESH)

    def across(l, dz):
        slab_copy(l, zz(dz), c).start()

    def got_across(l):
        for zs in range(nz):
            slab_copy(l, zs, 1 - c).wait_recv()

    far = nz // 2

    def goes_up(dy):
        return dy in (0, 3)

    def z_steps(l, dz, dy, up):
        if FAST[l]:
            return {0: (2, -2, 1, -1), -2: (2, 1) if up else (1,), 2: (-1,) if up else (-2, -1)}.get(dz, ())
        if dz == 0:
            return (1, -1)
        if dz < 0:
            return (1,) if -dz < far - 1 + up else ()
        return (-1,) if dz < far - up else ()

    seen = {}

    def pass_on(core, event):
        l, dz, dy = event // 100, event // 10 % 10 - 3, event % 10
        if (dz, dy) == (0, 0):
            w_loads[l].wait()
        else:
            got(l, dz, dy)
        if core == 0:
            if dy == 0:
                for step in z_steps(l, dz, dy, 1):
                    z_out(l, dz, dy, step)
                y_out(l, dz)
        else:
            if (dz, dy) == (0, 0):
                y_out(l, dz)
            for step in z_steps(l, dz, dy, int(goes_up(dy))):
                z_out(l, dz, dy, step)
        seen[core, l, dz] = seen.get((core, l, dz), 0) + 1
        if seen[core, l, dz] == NY:
            across(l, dz)

    def pass_all(core, events):
        for event in events:
            pass_on(core, event)

    def build_band():
        @pl.loop(0, tiles)
        def _(i):
            offset = (
                lax.broadcasted_iota(jnp.int32, (TILE, WINDOW), 1)
                - lax.broadcasted_iota(jnp.int32, (TILE, WINDOW), 0)
                - PAD
            )
            pos = base_pos + i * TILE + lax.broadcasted_iota(jnp.int32, (TILE, WINDOW), 0)
            count = jnp.minimum(pos + half, seq_total) - jnp.maximum(pos - half, 0)
            inverse = 1.0 / jnp.maximum(count, 1).astype(jnp.float32)
            mean = jnp.where((offset >= -half) & (offset < half), inverse, 0.0)
            band[i] = mean - jnp.where(offset == 0, 1.0, 0.0)

    def store_sums(layer, b, t, part):
        ss_own[layer, b, pl.ds(t, 1)] = jnp.sum(part.T, axis=0, keepdims=True)

    def square_sums():
        @pl.loop(0, BLOCKS)
        def _(b):
            for t in range(PER):
                row = pl.multiple_of(PAD + b * (PER * TILE), 64) + t * TILE
                part = jnp.zeros((TILE, 128), jnp.float32)
                for n in range(width // 128):
                    v = xs[0, pl.ds(row, TILE), pl.ds(n * 128, 128)].astype(jnp.float32)
                    part = part + v * v
                store_sums(0, b, t, part)

    def ss_copy(layer, b, p):
        return pltpu.make_async_remote_copy(
            ss_own.at[layer, b], ss_in.at[layer, p - 1, b], ss_send.at[layer, p - 1, b], ss_recv.at[layer, p - 1, b],
            device_id=(sp, lax.rem(tp + p, n_tp)), device_id_type=MESH)

    def send_sums(layer, b):
        for p in range(1, n_tp):
            ss_copy(layer, b, p).start()

    def factors(layer, b):
        for p in range(1, n_tp):
            ss_copy(layer, b, p).wait()
        total = ss_own[layer, b]
        for p in range(1, n_tp):
            total = total + ss_in[layer, p - 1, b]
        factor = lax.rsqrt(total / D + NORM_EPS)
        tile = b * PER + lax.broadcasted_iota(jnp.int32, total.shape, 0)
        pos = base_pos + tile * TILE + lax.broadcasted_iota(jnp.int32, total.shape, 1)
        factor = jnp.where((pos >= 0) & (pos < seq_total), factor, 0.0)
        fac[pl.ds(8 + b * PER, PER)] = factor[:PER]

    def pool(layer, b):
        low = pltpu.roll(fac[pl.ds(7 + b * PER, PER + 1)], PAD, 1)
        high = pltpu.roll(fac[pl.ds(8 + b * PER, PER + 1)], PAD, 1)
        lane = lax.broadcasted_iota(jnp.int32, low.shape, 1)
        shifted = jnp.where(lane < PAD, low, high)
        for t in range(PER):
            i = b * PER + t
            factor = jnp.concatenate([shifted[t : t + 1], shifted[t + 1 : t + 2]], axis=1)
            weights = (band[i] * factor).astype(jnp.bfloat16)
            for n in range(width // 256):
                cols = pl.ds(n * 256, 256)
                window = xs[layer % 2, pl.ds(i * TILE, WINDOW), cols]
                sums = jnp.dot(weights, window, preferred_element_type=jnp.float32)
                g = gain_ref[layer : layer + 1, cols].astype(jnp.float32)
                ps[pl.ds(i * TILE, TILE), cols] = (sums * g).astype(jnp.bfloat16)

    def mixed_block(layer, first_row, block, n):
        cols = pl.ds(n * 256, 256)
        weight = ws[layer, :, :, :, :, cols].reshape(width, 256)
        branch = jnp.dot(ps[pl.ds(first_row, block)], weight, preferred_element_type=jnp.float32)
        s = scale_ref[layer : layer + 1, cols].astype(jnp.float32)
        old = xs[layer % 2, pl.ds(PAD + first_row, block), cols].astype(jnp.float32)
        return (old + branch * s).astype(jnp.bfloat16)

    def mix(layer, b):
        block = PER * TILE
        part = jnp.zeros((block, 128), jnp.float32)
        for n in range(width // 256):
            mixed = mixed_block(layer, b * block, block, n)
            xs[(layer + 1) % 2, pl.ds(PAD + b * block, block), pl.ds(n * 256, 256)] = mixed
            v = mixed.astype(jnp.float32)
            sq = v * v
            part = part + sq[:, :128] + sq[:, 128:]
        for t in range(PER):
            store_sums(layer + 1, b, t, part[t * TILE : (t + 1) * TILE])
        send_sums(layer + 1, b)

    def mix_out(layer, b):
        first = max(b * PER * TILE, PAD)
        block = min((b + 1) * PER * TILE, PAD + rows) - first
        for n in range(width // 256):
            out_ref[pl.ds(first - PAD, block), pl.ds(n * 256, 256)] = mixed_block(layer, first, block, n)

    def start_work():
        x_load.wait()
        gain_load.wait()
        scale_load.wait()
        pl.when(has_prev)(lambda: to_next.wait_recv())
        pl.when(has_next)(lambda: to_prev.wait_recv())

    last = layers - 1

    def task(name):
        kind, l, b = name[0], int(name[1]), int(name[2])
        if kind == "b":
            start_halo()
            build_band()
        elif kind == "x":
            start_work()
            square_sums()
            for block in range(BLOCKS):
                send_sums(0, block)
        elif kind == "q":
            if b == 0:
                factors(l, 0)
            if b < BLOCKS - 1:
                factors(l, b + 1)
            pool(l, b)
        elif kind == "m":
            if b == 0:
                got_across(l)
            (mix_out if l == last else mix)(l, b)

    for first, second, name in PLAN:
        if first:
            pl.when(c == 0)(functools.partial(pass_all, 0, first))
        if second:
            pl.when(c == 1)(functools.partial(pass_all, 1, second))
        if name:
            task(name)
    pl.when(has_next)(lambda: to_next.wait_send())
    pl.when(has_prev)(lambda: to_prev.wait_send())

    def drain(l, way, refs):
        pltpu.make_async_remote_copy(
            refs, refs, w_send.at[l, way], w_recv.at[l, 0], device_id=partner, device_id_type=MESH).wait_send()

    for l in range(layers):
        drain(l, ACROSS, ws.at[l, :, :, 0])

        @pl.when(c == 0)
        def _():
            drain(l, ALONG_Z, ws.at[l, pl.ds(0, nz - 1), 0, 0])
            drain(l, ALONG_Y, ws.at[l, :, pl.ds(0, NY - 1), 0])

        @pl.when(c == 1)
        def _():
            drain(l, ALONG_Z, ws.at[l, pl.ds(0, nz - 1), :, 0])
            drain(l, ALONG_Y, ws.at[l, 0, pl.ds(0, NY - 1), 0])


def solution(mesh):
    n_sp, n_tp = mesh.shape["sp"], mesh.shape["tp"]

    def local(stream, norm_gain, pool_weight, pool_scale):
        rows, _ = stream.shape
        layers, per_dev, shard_rows, width = pool_weight.shape
        assert per_dev == 1 and n_tp == POOL_GROUPS and n_sp % (4 * NY) == 0
        total_rows = rows + 2 * PAD
        dma = pltpu.SemaphoreType.DMA
        hbm = pl.BlockSpec(memory_space=pltpu.HBM)
        return pl.pallas_call(
            functools.partial(kernel, (layers, rows, width, shard_rows, n_sp, n_tp)),
            out_shape=pltpu.VMEM((rows, width), jnp.bfloat16),
            in_specs=[hbm] * 4,
            out_specs=pl.BlockSpec(memory_space=pltpu.VMEM),
            scratch_shapes=[
                pltpu.VMEM((layers, width), jnp.bfloat16),
                pltpu.VMEM((layers, width), jnp.bfloat16),
                pltpu.VMEM((2, total_rows + 2 * PAD, width), jnp.bfloat16),
                pltpu.VMEM((total_rows, width), jnp.bfloat16),
                pltpu.VMEM((layers, n_sp // (2 * NY), NY, 2, shard_rows, width), jnp.bfloat16),
                pltpu.VMEM((total_rows // TILE, TILE, WINDOW), jnp.float32),
                pltpu.VMEM((24, TILE), jnp.float32),
                pltpu.VMEM((layers, BLOCKS, 8, TILE), jnp.float32),
                pltpu.VMEM((layers, n_tp - 1, BLOCKS, 8, TILE), jnp.float32),
                dma((layers + 3,)),
                dma((2,)),
                dma((2,)),
                dma((layers, n_tp - 1, BLOCKS)),
                dma((layers, n_tp - 1, BLOCKS)),
                dma((layers, 3)),
                dma((layers, n_sp)),
            ],
            compiler_params=pltpu.CompilerParams(
                collective_id=0, has_side_effects=True, vmem_limit_bytes=60 * 2**20
            ),
        )(stream, pool_weight, norm_gain, pool_scale)

    placed = (P("sp", "tp"), P(None, "tp"), P(None, "tp", "sp", None), P(None, "tp"))
    return jax.shard_map(
        local, mesh=mesh, in_specs=placed, out_specs=P("sp", "tp"), check_vma=False
    )
```

```python
import functools

import jax
import jax.numpy as jnp
from jax import lax
from jax.experimental import pallas as pl
from jax.experimental.pallas import tpu as pltpu
from jax.sharding import PartitionSpec as P

D = 4096
POOL_GROUPS = 4
NORM_EPS = 1e-06
PAD = 64
HALO = 32
TILE = 128
WINDOW = TILE + 2 * PAD
PER = 3
BLOCKS = 3
NY = 4
FAST = (False, False, False)
PLAN = (
    ((30,), (30,), 'b00'),
    ((20, 40, 31, 33, 130), (20, 40, 33, 31, 130), 'x00'),
    ((32, 23, 21, 10, 43, 41, 50, 230, 22, 120, 140, 131, 133), (32, 10, 50, 43, 23, 21, 41, 230, 131, 133, 120, 22, 42, 140), 'q00'),
    ((42, 132), (0, 13, 53, 60, 132, 51), 'q01'),
    ((13, 11), (11,), 'q02'),
    ((0, 60, 51, 53, 220, 240, 12, 231, 233, 52, 110, 232, 123, 121, 150, 143, 141, 122, 142, 3, 1, 70, 61, 63, 250, 223, 221, 2, 210, 243, 241, 62, 222, 113, 111, 242, 100, 160, 153, 151, 112, 73, 71, 152, 253, 251, 260, 213, 211, 72, 200, 252, 103, 101, 212, 163, 161), (220, 240, 121, 141, 231, 233, 143, 123, 110, 52, 232, 12, 150, 70, 63, 3, 142, 122, 61, 1, 250, 210, 151, 241, 111, 243, 221, 153, 223, 62, 113, 242, 100, 160, 222, 152, 2, 71, 73, 260, 112, 161, 200, 101, 251, 253, 211, 163, 213, 72, 103, 252), 'm00'),
    ((170, 102, 162, 201, 203, 261, 263), (162, 170, 102, 171, 212, 261, 263, 270), 'm01'),
    ((270, 202, 262), (203, 262, 201, 173), 'm02'),
    ((171, 173, 172, 273, 271), (172, 202, 271, 273, 272), 'q10'),
    ((), (), 'm10'),
    ((272,), (), 'q11'),
    ((), (), 'm11'),
    ((), (), 'q12'),
    ((), (), 'm12'),
    ((), (), 'q20'),
    ((), (), 'm20'),
    ((), (), 'q21'),
    ((), (), 'm21'),
    ((), (), 'q22'),
    ((), (), 'm22'),
    ((), (), ''),
)
ALONG_Z, ALONG_Y, ACROSS = 0, 1, 2
MESH = pl.DeviceIdType.MESH


def kernel(cfg, x_hbm, w_hbm, gain_hbm, scale_hbm, out_ref, gain_ref, scale_ref, xs, ps, ws, band, fac, ss_own, ss_in,
           load_sem, halo_send, halo_recv, ss_send, ss_recv, w_send, w_recv):
    layers, rows, width, shard_rows, n_sp, n_tp = cfg
    sp, tp = lax.axis_index("sp"), lax.axis_index("tp")
    nz = n_sp // (2 * NY)
    z, y, c = sp // (2 * NY), (sp // 2) % NY, sp % 2
    tiles = (rows + 2 * PAD) // TILE
    seq_total = rows * n_sp
    base_pos = sp * rows - PAD
    half = jnp.left_shift(jnp.int32(1), tp)
    has_prev, has_next = sp > 0, sp < n_sp - 1

    x_load = pltpu.make_async_copy(x_hbm, xs.at[0, pl.ds(2 * PAD, rows)], load_sem.at[layers])
    w_loads = [pltpu.make_async_copy(w_hbm.at[l, 0], ws.at[l, z, y, c], load_sem.at[l]) for l in range(layers)]
    gain_load = pltpu.make_async_copy(gain_hbm, gain_ref, load_sem.at[layers + 1])
    scale_load = pltpu.make_async_copy(scale_hbm, scale_ref, load_sem.at[layers + 2])
    w_loads[0].start()
    x_load.start()
    for l in range(1, layers):
        w_loads[l].start()
    gain_load.start()
    scale_load.start()

    def at_z(step):
        return ((lax.rem(z + step + nz, nz) * NY + y) * 2 + c, tp)

    def at_y(step):
        return ((z * NY + lax.rem(y + step + NY, NY)) * 2 + c, tp)

    partner = ((z * NY + y) * 2 + 1 - c, tp)

    barrier = pltpu.get_barrier_semaphore()

    def greet(device):
        pl.semaphore_signal(barrier, inc=1, device_id=device, device_id_type=MESH)

    for device in [at_z(1), at_z(-1), at_y(1), at_y(-1), at_y(2), partner]:
        greet(device)
    for p in range(1, n_tp):
        greet((sp, lax.rem(tp + p, n_tp)))
    pl.when(has_prev)(lambda: greet((sp - 1, tp)))
    pl.when(has_next)(lambda: greet((sp + 1, tp)))
    expected = 6 + n_tp - 1 + has_prev.astype(jnp.int32) + has_next.astype(jnp.int32)

    zero = jnp.zeros((2 * PAD, width), jnp.bfloat16)
    xs[0, pl.ds(0, 2 * PAD - HALO)] = zero[: 2 * PAD - HALO]
    xs[0, pl.ds(2 * PAD + rows + HALO, 2 * PAD - HALO)] = zero[: 2 * PAD - HALO]
    xs[1, pl.ds(0, PAD)] = zero[:PAD]
    xs[1, pl.ds(3 * PAD + rows, PAD)] = zero[:PAD]

    @pl.when(jnp.logical_not(has_prev))
    def _():
        xs[0, pl.ds(2 * PAD - HALO, HALO)] = zero[:HALO]

    @pl.when(jnp.logical_not(has_next))
    def _():
        xs[0, pl.ds(2 * PAD + rows, HALO)] = zero[:HALO]

    ss_own[...] = jnp.zeros(ss_own.shape, jnp.float32)
    fac[...] = jnp.zeros(fac.shape, jnp.float32)

    pl.semaphore_wait(barrier, expected)

    to_next = pltpu.make_async_remote_copy(
        x_hbm.at[pl.ds(rows - HALO, HALO)], xs.at[0, pl.ds(2 * PAD - HALO, HALO)],
        halo_send.at[0], halo_recv.at[0], device_id=(sp + 1, tp), device_id_type=MESH)
    to_prev = pltpu.make_async_remote_copy(
        x_hbm.at[pl.ds(0, HALO)], xs.at[0, pl.ds(2 * PAD + rows, HALO)],
        halo_send.at[1], halo_recv.at[1], device_id=(sp - 1, tp), device_id_type=MESH)

    def start_halo():
        pl.when(has_next)(lambda: to_next.start())
        pl.when(has_prev)(lambda: to_prev.start())

    def zz(step):
        return lax.rem(z + step + nz, nz)

    def yy(step):
        return lax.rem(y + step + NY, NY)

    def shard_copy(l, dz, dy, device, way):
        zs, ys = zz(dz), yy(dy)
        piece = ws.at[l, zs, ys, c]
        return pltpu.make_async_remote_copy(
            piece, piece, w_send.at[l, way], w_recv.at[l, (zs * NY + ys) * 2 + c],
            device_id=device, device_id_type=MESH)

    def z_out(l, dz, dy, step):
        shard_copy(l, dz, dy, at_z(step), ALONG_Z).start()

    def y_out(l, dz):
        for step in (2, 1, -1):
            shard_copy(l, dz, 0, at_y(step), ALONG_Y).start()

    def got(l, dz, dy):
        shard_copy(l, dz, dy, partner, ALONG_Z).wait_recv()

    def slab_copy(l, zs, core):
        slab = ws.at[l, zs, :, core]
        return pltpu.make_async_remote_copy(
            slab, slab, w_send.at[l, ACROSS], w_recv.at[l, zs * NY * 2 + core],
            device_id=partner, device_id_type=MESH)

    def across(l, dz):
        slab_copy(l, zz(dz), c).start()

    def got_across(l):
        for zs in range(nz):
            slab_copy(l, zs, 1 - c).wait_recv()

    far = nz // 2

    def goes_up(dy):
        return dy in (0, 3)

    def z_steps(l, dz, dy, up):
        if FAST[l]:
            return {0: (2, -2, 1, -1), -2: (2, 1) if up else (1,), 2: (-1,) if up else (-2, -1)}.get(dz, ())
        if dz == 0:
            return (1, -1)
        if dz < 0:
            return (1,) if -dz < far - 1 + up else ()
        return (-1,) if dz < far - up else ()

    seen = {}

    def pass_on(core, event):
        l, dz, dy = event // 100, event // 10 % 10 - 3, event % 10
        if (dz, dy) == (0, 0):
            w_loads[l].wait()
        else:
            got(l, dz, dy)
        if core == 0:
            if dy == 0:
                for step in z_steps(l, dz, dy, 1):
                    z_out(l, dz, dy, step)
                y_out(l, dz)
        else:
            if (dz, dy) == (0, 0):
                y_out(l, dz)
            for step in z_steps(l, dz, dy, int(goes_up(dy))):
                z_out(l, dz, dy, step)
        seen[core, l, dz] = seen.get((core, l, dz), 0) + 1
        if seen[core, l, dz] == NY:
            across(l, dz)

    def pass_all(core, events):
        for event in events:
            pass_on(core, event)

    def build_band():
        @pl.loop(0, tiles)
        def _(i):
            offset = (
                lax.broadcasted_iota(jnp.int32, (TILE, WINDOW), 1)
                - lax.broadcasted_iota(jnp.int32, (TILE, WINDOW), 0)
                - PAD
            )
            pos = base_pos + i * TILE + lax.broadcasted_iota(jnp.int32, (TILE, WINDOW), 0)
            count = jnp.minimum(pos + half, seq_total) - jnp.maximum(pos - half, 0)
            inverse = 1.0 / jnp.maximum(count, 1).astype(jnp.float32)
            mean = jnp.where((offset >= -half) & (offset < half), inverse, 0.0)
            band[i] = mean - jnp.where(offset == 0, 1.0, 0.0)

    def store_sums(layer, b, t, part):
        ss_own[layer, b, pl.ds(t, 1)] = jnp.sum(part.T, axis=0, keepdims=True)

    def square_sums():
        @pl.loop(0, BLOCKS)
        def _(b):
            for t in range(PER):
                row = pl.multiple_of(PAD + b * (PER * TILE), 64) + t * TILE
                part = jnp.zeros((TILE, 128), jnp.float32)
                for n in range(width // 128):
                    v = xs[0, pl.ds(row, TILE), pl.ds(n * 128, 128)].astype(jnp.float32)
                    part = part + v * v
                store_sums(0, b, t, part)

    def ss_copy(layer, b, p):
        return pltpu.make_async_remote_copy(
            ss_own.at[layer, b], ss_in.at[layer, p - 1, b], ss_send.at[layer, p - 1, b], ss_recv.at[layer, p - 1, b],
            device_id=(sp, lax.rem(tp + p, n_tp)), device_id_type=MESH)

    def send_sums(layer, b):
        for p in range(1, n_tp):
            ss_copy(layer, b, p).start()

    def factors(layer, b):
        for p in range(1, n_tp):
            ss_copy(layer, b, p).wait()
        total = ss_own[layer, b]
        for p in range(1, n_tp):
            total = total + ss_in[layer, p - 1, b]
        factor = lax.rsqrt(total / D + NORM_EPS)
        tile = b * PER + lax.broadcasted_iota(jnp.int32, total.shape, 0)
        pos = base_pos + tile * TILE + lax.broadcasted_iota(jnp.int32, total.shape, 1)
        factor = jnp.where((pos >= 0) & (pos < seq_total), factor, 0.0)
        fac[pl.ds(8 + b * PER, PER)] = factor[:PER]

    def pool(layer, b):
        low = pltpu.roll(fac[pl.ds(7 + b * PER, PER + 1)], PAD, 1)
        high = pltpu.roll(fac[pl.ds(8 + b * PER, PER + 1)], PAD, 1)
        lane = lax.broadcasted_iota(jnp.int32, low.shape, 1)
        shifted = jnp.where(lane < PAD, low, high)
        for t in range(PER):
            i = b * PER + t
            factor = jnp.concatenate([shifted[t : t + 1], shifted[t + 1 : t + 2]], axis=1)
            weights = (band[i] * factor).astype(jnp.bfloat16)
            for n in range(width // 256):
                cols = pl.ds(n * 256, 256)
                window = xs[layer % 2, pl.ds(i * TILE, WINDOW), cols]
                sums = jnp.dot(weights, window, preferred_element_type=jnp.float32)
                g = gain_ref[layer : layer + 1, cols].astype(jnp.float32)
                ps[pl.ds(i * TILE, TILE), cols] = (sums * g).astype(jnp.bfloat16)

    def mixed_block(layer, first_row, block, n):
        cols = pl.ds(n * 256, 256)
        weight = ws[layer, :, :, :, :, cols].reshape(width, 256)
        branch = jnp.dot(ps[pl.ds(first_row, block)], weight, preferred_element_type=jnp.float32)
        s = scale_ref[layer : layer + 1, cols].astype(jnp.float32)
        old = xs[layer % 2, pl.ds(PAD + first_row, block), cols].astype(jnp.float32)
        return (old + branch * s).astype(jnp.bfloat16)

    def mix(layer, b):
        block = PER * TILE
        part = jnp.zeros((block, 128), jnp.float32)
        for n in range(width // 256):
            mixed = mixed_block(layer, b * block, block, n)
            xs[(layer + 1) % 2, pl.ds(PAD + b * block, block), pl.ds(n * 256, 256)] = mixed
            v = mixed.astype(jnp.float32)
            sq = v * v
            part = part + sq[:, :128] + sq[:, 128:]
        for t in range(PER):
            store_sums(layer + 1, b, t, part[t * TILE : (t + 1) * TILE])
        send_sums(layer + 1, b)

    def mix_out(layer, b):
        first = max(b * PER * TILE, PAD)
        block = min((b + 1) * PER * TILE, PAD + rows) - first
        for n in range(width // 256):
            out_ref[pl.ds(first - PAD, block), pl.ds(n * 256, 256)] = mixed_block(layer, first, block, n)

    def start_work():
        x_load.wait()
        gain_load.wait()
        scale_load.wait()
        pl.when(has_prev)(lambda: to_next.wait_recv())
        pl.when(has_next)(lambda: to_prev.wait_recv())

    last = layers - 1

    def task(name):
        kind, l, b = name[0], int(name[1]), int(name[2])
        if kind == "b":
            start_halo()
            build_band()
        elif kind == "x":
            start_work()
            square_sums()
            for block in range(BLOCKS):
                send_sums(0, block)
        elif kind == "q":
            if b == 0:
                factors(l, 0)
            if b < BLOCKS - 1:
                factors(l, b + 1)
            pool(l, b)
        elif kind == "m":
            if b == 0:
                got_across(l)
            (mix_out if l == last else mix)(l, b)

    for first, second, name in PLAN:
        if first:
            pl.when(c == 0)(functools.partial(pass_all, 0, first))
        if second:
            pl.when(c == 1)(functools.partial(pass_all, 1, second))
        if name:
            task(name)
    pl.when(has_next)(lambda: to_next.wait_send())
    pl.when(has_prev)(lambda: to_prev.wait_send())

    def drain(l, way, refs):
        pltpu.make_async_remote_copy(
            refs, refs, w_send.at[l, way], w_recv.at[l, 0], device_id=partner, device_id_type=MESH).wait_send()

    for l in range(layers):
        drain(l, ACROSS, ws.at[l, :, :, 0])

        @pl.when(c == 0)
        def _():
            drain(l, ALONG_Z, ws.at[l, pl.ds(0, nz - 1), 0, 0])
            drain(l, ALONG_Y, ws.at[l, :, pl.ds(0, NY - 1), 0])

        @pl.when(c == 1)
        def _():
            drain(l, ALONG_Z, ws.at[l, pl.ds(0, nz - 1), :, 0])
            drain(l, ALONG_Y, ws.at[l, 0, pl.ds(0, NY - 1), 0])


def solution(mesh):
    n_sp, n_tp = mesh.shape["sp"], mesh.shape["tp"]

    def local(stream, norm_gain, pool_weight, pool_scale):
        rows, _ = stream.shape
        layers, per_dev, shard_rows, width = pool_weight.shape
        assert per_dev == 1 and n_tp == POOL_GROUPS and n_sp % (4 * NY) == 0
        total_rows = rows + 2 * PAD
        dma = pltpu.SemaphoreType.DMA
        hbm = pl.BlockSpec(memory_space=pltpu.HBM)
        return pl.pallas_call(
            functools.partial(kernel, (layers, rows, width, shard_rows, n_sp, n_tp)),
            out_shape=pltpu.VMEM((rows, width), jnp.bfloat16),
            in_specs=[hbm] * 4,
            out_specs=pl.BlockSpec(memory_space=pltpu.VMEM),
            scratch_shapes=[
                pltpu.VMEM((layers, width), jnp.bfloat16),
                pltpu.VMEM((layers, width), jnp.bfloat16),
                pltpu.VMEM((2, total_rows + 2 * PAD, width), jnp.bfloat16),
                pltpu.VMEM((total_rows, width), jnp.bfloat16),
                pltpu.VMEM((layers, n_sp // (2 * NY), NY, 2, shard_rows, width), jnp.bfloat16),
                pltpu.VMEM((total_rows // TILE, TILE, WINDOW), jnp.float32),
                pltpu.VMEM((24, TILE), jnp.float32),
                pltpu.VMEM((layers, BLOCKS, 8, TILE), jnp.float32),
                pltpu.VMEM((layers, n_tp - 1, BLOCKS, 8, TILE), jnp.float32),
                dma((layers + 3,)),
                dma((2,)),
                dma((2,)),
                dma((layers, n_tp - 1, BLOCKS)),
                dma((layers, n_tp - 1, BLOCKS)),
                dma((layers, 3)),
                dma((layers, n_sp)),
            ],
            compiler_params=pltpu.CompilerParams(
                collective_id=0, has_side_effects=True, vmem_limit_bytes=60 * 2**20
            ),
        )(stream, pool_weight, norm_gain, pool_scale)

    placed = (P("sp", "tp"), P(None, "tp"), P(None, "tp", "sp", None), P(None, "tp"))
    return jax.shard_map(
        local, mesh=mesh, in_specs=placed, out_specs=P("sp", "tp"), check_vma=False
    )
```

```python
import functools

import jax
import jax.numpy as jnp
from jax import lax
from jax.experimental import pallas as pl
from jax.experimental.pallas import tpu as pltpu
from jax.sharding import PartitionSpec as P

D = 4096
POOL_GROUPS = 4
NORM_EPS = 1e-06
PAD = 64
HALO = 32
TILE = 128
WINDOW = TILE + 2 * PAD
PER = 3
BLOCKS = 3
NY = 4
FAST = (False, False, False)
PLAN = (
    ((30,), (30,), 'b00'),
    ((20, 40, 31, 33, 130), (20, 40, 33, 31, 130), 'x00'),
    ((32, 23, 21, 10, 43, 41, 50, 230, 22, 120, 140, 131, 133), (32, 10, 50, 43, 23, 21, 41, 230, 131, 133, 120, 22, 42, 140), 'q00'),
    ((42, 132), (0, 13, 53, 60, 132, 51), 'q01'),
    ((13, 11), (11,), 'q02'),
    ((0, 60, 51, 53, 220, 240, 12, 231, 233, 52, 110, 232, 123, 121, 150, 143, 141, 122, 142, 3, 1, 70, 61, 63, 250, 223, 221, 2, 210, 243, 241, 62, 222, 113, 111, 242, 100, 160, 153, 151, 112, 73, 71, 152, 253, 251, 260, 213, 211, 72, 200, 252, 103, 101, 212, 163, 161), (220, 240, 121, 141, 231, 233, 143, 123, 110, 52, 232, 12, 150, 70, 63, 3, 142, 122, 61, 1, 250, 210, 151, 241, 111, 243, 221, 153, 223, 62, 113, 242, 100, 160, 222, 152, 2, 71, 73, 260, 112, 161, 200, 101, 251, 253, 211, 163, 213, 72, 103, 252), 'm00'),
    ((170, 102, 162, 201, 203, 261, 263), (162, 170, 102, 171, 212, 261, 263, 270), 'm01'),
    ((270, 202, 262), (203, 262, 201, 173), 'm02'),
    ((171, 173, 172, 273, 271), (172, 202, 271, 273, 272), 'q10'),
    ((), (), 'm10'),
    ((272,), (), 'q11'),
    ((), (), 'm11'),
    ((), (), 'q12'),
    ((), (), 'm12'),
    ((), (), 'q20'),
    ((), (), 'm20'),
    ((), (), 'q21'),
    ((), (), 'm21'),
    ((), (), 'q22'),
    ((), (), 'm22'),
    ((), (), ''),
)
ALONG_Z, ALONG_Y, ACROSS = 0, 1, 2
MESH = pl.DeviceIdType.MESH


def kernel(cfg, x_hbm, w_hbm, gain_hbm, scale_hbm, out_ref, gain_ref, scale_ref, xs, ps, ws, band, fac, ss_own, ss_in,
           load_sem, halo_send, halo_recv, ss_send, ss_recv, w_send, w_recv):
    layers, rows, width, shard_rows, n_sp, n_tp = cfg
    sp, tp = lax.axis_index("sp"), lax.axis_index("tp")
    nz = n_sp // (2 * NY)
    z, y, c = sp // (2 * NY), (sp // 2) % NY, sp % 2
    tiles = (rows + 2 * PAD) // TILE
    seq_total = rows * n_sp
    base_pos = sp * rows - PAD
    half = jnp.left_shift(jnp.int32(1), tp)
    has_prev, has_next = sp > 0, sp < n_sp - 1

    x_load = pltpu.make_async_copy(x_hbm, xs.at[0, pl.ds(2 * PAD, rows)], load_sem.at[layers])
    w_loads = [pltpu.make_async_copy(w_hbm.at[l, 0], ws.at[l, z, y, c], load_sem.at[l]) for l in range(layers)]
    gain_load = pltpu.make_async_copy(gain_hbm, gain_ref, load_sem.at[layers + 1])
    scale_load = pltpu.make_async_copy(scale_hbm, scale_ref, load_sem.at[layers + 2])
    w_loads[0].start()
    x_load.start()
    for l in range(1, layers):
        w_loads[l].start()
    gain_load.start()
    scale_load.start()

    def at_z(step):
        return ((lax.rem(z + step + nz, nz) * NY + y) * 2 + c, tp)

    def at_y(step):
        return ((z * NY + lax.rem(y + step + NY, NY)) * 2 + c, tp)

    partner = ((z * NY + y) * 2 + 1 - c, tp)

    barrier = pltpu.get_barrier_semaphore()

    def greet(device):
        pl.semaphore_signal(barrier, inc=1, device_id=device, device_id_type=MESH)

    for device in [at_z(1), at_z(-1), at_y(1), at_y(-1), at_y(2), partner]:
        greet(device)
    for p in range(1, n_tp):
        greet((sp, lax.rem(tp + p, n_tp)))
    pl.when(has_prev)(lambda: greet((sp - 1, tp)))
    pl.when(has_next)(lambda: greet((sp + 1, tp)))
    expected = 6 + n_tp - 1 + has_prev.astype(jnp.int32) + has_next.astype(jnp.int32)

    zero = jnp.zeros((2 * PAD, width), jnp.bfloat16)
    xs[0, pl.ds(0, 2 * PAD - HALO)] = zero[: 2 * PAD - HALO]
    xs[0, pl.ds(2 * PAD + rows + HALO, 2 * PAD - HALO)] = zero[: 2 * PAD - HALO]
    xs[1, pl.ds(0, PAD)] = zero[:PAD]
    xs[1, pl.ds(3 * PAD + rows, PAD)] = zero[:PAD]

    @pl.when(jnp.logical_not(has_prev))
    def _():
        xs[0, pl.ds(2 * PAD - HALO, HALO)] = zero[:HALO]

    @pl.when(jnp.logical_not(has_next))
    def _():
        xs[0, pl.ds(2 * PAD + rows, HALO)] = zero[:HALO]

    ss_own[...] = jnp.zeros(ss_own.shape, jnp.float32)
    fac[...] = jnp.zeros(fac.shape, jnp.float32)

    def build_band():
        @pl.loop(0, tiles)
        def _(i):
            offset = (
                lax.broadcasted_iota(jnp.int32, (TILE, WINDOW), 1)
                - lax.broadcasted_iota(jnp.int32, (TILE, WINDOW), 0)
                - PAD
            )
            pos = base_pos + i * TILE + lax.broadcasted_iota(jnp.int32, (TILE, WINDOW), 0)
            count = jnp.minimum(pos + half, seq_total) - jnp.maximum(pos - half, 0)
            inverse = 1.0 / jnp.maximum(count, 1).astype(jnp.float32)
            mean = jnp.where((offset >= -half) & (offset < half), inverse, 0.0)
            band[i] = mean - jnp.where(offset == 0, 1.0, 0.0)

    build_band()
    pl.semaphore_wait(barrier, expected)

    to_next = pltpu.make_async_remote_copy(
        x_hbm.at[pl.ds(rows - HALO, HALO)], xs.at[0, pl.ds(2 * PAD - HALO, HALO)],
        halo_send.at[0], halo_recv.at[0], device_id=(sp + 1, tp), device_id_type=MESH)
    to_prev = pltpu.make_async_remote_copy(
        x_hbm.at[pl.ds(0, HALO)], xs.at[0, pl.ds(2 * PAD + rows, HALO)],
        halo_send.at[1], halo_recv.at[1], device_id=(sp - 1, tp), device_id_type=MESH)

    def start_halo():
        pl.when(has_next)(lambda: to_next.start())
        pl.when(has_prev)(lambda: to_prev.start())

    def zz(step):
        return lax.rem(z + step + nz, nz)

    def yy(step):
        return lax.rem(y + step + NY, NY)

    def shard_copy(l, dz, dy, device, way):
        zs, ys = zz(dz), yy(dy)
        piece = ws.at[l, zs, ys, c]
        return pltpu.make_async_remote_copy(
            piece, piece, w_send.at[l, way], w_recv.at[l, (zs * NY + ys) * 2 + c],
            device_id=device, device_id_type=MESH)

    def z_out(l, dz, dy, step):
        shard_copy(l, dz, dy, at_z(step), ALONG_Z).start()

    def y_out(l, dz):
        for step in (1, -1, 2):
            shard_copy(l, dz, 0, at_y(step), ALONG_Y).start()

    def got(l, dz, dy):
        shard_copy(l, dz, dy, partner, ALONG_Z).wait_recv()

    def slab_copy(l, zs, core):
        slab = ws.at[l, zs, :, core]
        return pltpu.make_async_remote_copy(
            slab, slab, w_send.at[l, ACROSS], w_recv.at[l, zs * NY * 2 + core],
            device_id=partner, device_id_type=MESH)

    def across(l, dz):
        slab_copy(l, zz(dz), c).start()

    def got_across(l):
        for zs in range(nz):
            slab_copy(l, zs, 1 - c).wait_recv()

    far = nz // 2

    def goes_up(dy):
        return dy in (0, 3)

    def z_steps(l, dz, dy, up):
        if FAST[l]:
            return {0: (2, -2, 1, -1), -2: (2, 1) if up else (1,), 2: (-1,) if up else (-2, -1)}.get(dz, ())
        if dz == 0:
            return (1, -1)
        if dz < 0:
            return (1,) if -dz < far - 1 + up else ()
        return (-1,) if dz < far - up else ()

    seen = {}

    def pass_on(core, event):
        l, dz, dy = event // 100, event // 10 % 10 - 3, event % 10
        if (dz, dy) == (0, 0):
            w_loads[l].wait()
        else:
            got(l, dz, dy)
        if core == 0:
            if dy == 0:
                for step in z_steps(l, dz, dy, 1):
                    z_out(l, dz, dy, step)
                y_out(l, dz)
        else:
            if (dz, dy) == (0, 0):
                y_out(l, dz)
            for step in z_steps(l, dz, dy, int(goes_up(dy))):
                z_out(l, dz, dy, step)
        seen[core, l, dz] = seen.get((core, l, dz), 0) + 1
        if seen[core, l, dz] == NY:
            across(l, dz)

    def pass_all(core, events):
        for event in events:
            pass_on(core, event)

    def store_sums(layer, b, t, part):
        ss_own[layer, b, pl.ds(t, 1)] = jnp.sum(part.T, axis=0, keepdims=True)

    def square_sums():
        @pl.loop(0, BLOCKS)
        def _(b):
            for t in range(PER):
                row = pl.multiple_of(PAD + b * (PER * TILE), 64) + t * TILE
                part = jnp.zeros((TILE, 128), jnp.float32)
                for n in range(width // 128):
                    v = xs[0, pl.ds(row, TILE), pl.ds(n * 128, 128)].astype(jnp.float32)
                    part = part + v * v
                store_sums(0, b, t, part)

    def ss_copy(layer, b, p):
        return pltpu.make_async_remote_copy(
            ss_own.at[layer, b], ss_in.at[layer, p - 1, b], ss_send.at[layer, p - 1, b], ss_recv.at[layer, p - 1, b],
            device_id=(sp, lax.rem(tp + p, n_tp)), device_id_type=MESH)

    def send_sums(layer, b):
        for p in range(1, n_tp):
            ss_copy(layer, b, p).start()

    def factors(layer, b):
        for p in range(1, n_tp):
            ss_copy(layer, b, p).wait()
        total = ss_own[layer, b]
        for p in range(1, n_tp):
            total = total + ss_in[layer, p - 1, b]
        factor = lax.rsqrt(total / D + NORM_EPS)
        tile = b * PER + lax.broadcasted_iota(jnp.int32, total.shape, 0)
        pos = base_pos + tile * TILE + lax.broadcasted_iota(jnp.int32, total.shape, 1)
        factor = jnp.where((pos >= 0) & (pos < seq_total), factor, 0.0)
        fac[pl.ds(8 + b * PER, PER)] = factor[:PER]

    def pool(layer, b):
        low = pltpu.roll(fac[pl.ds(7 + b * PER, PER + 1)], PAD, 1)
        high = pltpu.roll(fac[pl.ds(8 + b * PER, PER + 1)], PAD, 1)
        lane = lax.broadcasted_iota(jnp.int32, low.shape, 1)
        shifted = jnp.where(lane < PAD, low, high)
        for t in range(PER):
            i = b * PER + t
            factor = jnp.concatenate([shifted[t : t + 1], shifted[t + 1 : t + 2]], axis=1)
            weights = (band[i] * factor).astype(jnp.bfloat16)
            for n in range(width // 256):
                cols = pl.ds(n * 256, 256)
                window = xs[layer % 2, pl.ds(i * TILE, WINDOW), cols]
                sums = jnp.dot(weights, window, preferred_element_type=jnp.float32)
                g = gain_ref[layer : layer + 1, cols].astype(jnp.float32)
                ps[pl.ds(i * TILE, TILE), cols] = (sums * g).astype(jnp.bfloat16)

    def mixed_block(layer, first_row, block, n):
        cols = pl.ds(n * 256, 256)
        weight = ws[layer, :, :, :, :, cols].reshape(width, 256)
        branch = jnp.dot(ps[pl.ds(first_row, block)], weight, preferred_element_type=jnp.float32)
        s = scale_ref[layer : layer + 1, cols].astype(jnp.float32)
        old = xs[layer % 2, pl.ds(PAD + first_row, block), cols].astype(jnp.float32)
        return (old + branch * s).astype(jnp.bfloat16)

    def mix(layer, b):
        block = PER * TILE
        part = jnp.zeros((block, 128), jnp.float32)
        for n in range(width // 256):
            mixed = mixed_block(layer, b * block, block, n)
            xs[(layer + 1) % 2, pl.ds(PAD + b * block, block), pl.ds(n * 256, 256)] = mixed
            v = mixed.astype(jnp.float32)
            sq = v * v
            part = part + sq[:, :128] + sq[:, 128:]
        for t in range(PER):
            store_sums(layer + 1, b, t, part[t * TILE : (t + 1) * TILE])
        send_sums(layer + 1, b)

    def mix_out(layer, b):
        first = max(b * PER * TILE, PAD)
        block = min((b + 1) * PER * TILE, PAD + rows) - first
        for n in range(width // 256):
            out_ref[pl.ds(first - PAD, block), pl.ds(n * 256, 256)] = mixed_block(layer, first, block, n)

    def start_work():
        x_load.wait()
        gain_load.wait()
        scale_load.wait()
        pl.when(has_prev)(lambda: to_next.wait_recv())
        pl.when(has_next)(lambda: to_prev.wait_recv())

    last = layers - 1

    def task(name):
        kind, l, b = name[0], int(name[1]), int(name[2])
        if kind == "b":
            start_halo()
        elif kind == "x":
            start_work()
            square_sums()
            for block in range(BLOCKS):
                send_sums(0, block)
        elif kind == "q":
            if b == 0:
                factors(l, 0)
            if b < BLOCKS - 1:
                factors(l, b + 1)
            pool(l, b)
        elif kind == "m":
            if b == 0:
                got_across(l)
            (mix_out if l == last else mix)(l, b)

    for first, second, name in PLAN:
        if first:
            pl.when(c == 0)(functools.partial(pass_all, 0, first))
        if second:
            pl.when(c == 1)(functools.partial(pass_all, 1, second))
        if name:
            task(name)
    pl.when(has_next)(lambda: to_next.wait_send())
    pl.when(has_prev)(lambda: to_prev.wait_send())

    def drain(l, way, refs):
        pltpu.make_async_remote_copy(
            refs, refs, w_send.at[l, way], w_recv.at[l, 0], device_id=partner, device_id_type=MESH).wait_send()

    for l in range(layers):
        drain(l, ACROSS, ws.at[l, :, :, 0])

        @pl.when(c == 0)
        def _():
            drain(l, ALONG_Z, ws.at[l, pl.ds(0, nz - 1), 0, 0])
            drain(l, ALONG_Y, ws.at[l, :, pl.ds(0, NY - 1), 0])

        @pl.when(c == 1)
        def _():
            drain(l, ALONG_Z, ws.at[l, pl.ds(0, nz - 1), :, 0])
            drain(l, ALONG_Y, ws.at[l, 0, pl.ds(0, NY - 1), 0])


def solution(mesh):
    n_sp, n_tp = mesh.shape["sp"], mesh.shape["tp"]

    def local(stream, norm_gain, pool_weight, pool_scale):
        rows, _ = stream.shape
        layers, per_dev, shard_rows, width = pool_weight.shape
        assert per_dev == 1 and n_tp == POOL_GROUPS and n_sp % (4 * NY) == 0
        total_rows = rows + 2 * PAD
        dma = pltpu.SemaphoreType.DMA
        hbm = pl.BlockSpec(memory_space=pltpu.HBM)
        return pl.pallas_call(
            functools.partial(kernel, (layers, rows, width, shard_rows, n_sp, n_tp)),
            out_shape=pltpu.VMEM((rows, width), jnp.bfloat16),
            in_specs=[hbm] * 4,
            out_specs=pl.BlockSpec(memory_space=pltpu.VMEM),
            scratch_shapes=[
                pltpu.VMEM((layers, width), jnp.bfloat16),
                pltpu.VMEM((layers, width), jnp.bfloat16),
                pltpu.VMEM((2, total_rows + 2 * PAD, width), jnp.bfloat16),
                pltpu.VMEM((total_rows, width), jnp.bfloat16),
                pltpu.VMEM((layers, n_sp // (2 * NY), NY, 2, shard_rows, width), jnp.bfloat16),
                pltpu.VMEM((total_rows // TILE, TILE, WINDOW), jnp.float32),
                pltpu.VMEM((24, TILE), jnp.float32),
                pltpu.VMEM((layers, BLOCKS, 8, TILE), jnp.float32),
                pltpu.VMEM((layers, n_tp - 1, BLOCKS, 8, TILE), jnp.float32),
                dma((layers + 3,)),
                dma((2,)),
                dma((2,)),
                dma((layers, n_tp - 1, BLOCKS)),
                dma((layers, n_tp - 1, BLOCKS)),
                dma((layers, 3)),
                dma((layers, n_sp)),
            ],
            compiler_params=pltpu.CompilerParams(
                collective_id=0, has_side_effects=True, vmem_limit_bytes=60 * 2**20
            ),
        )(stream, pool_weight, norm_gain, pool_scale)

    placed = (P("sp", "tp"), P(None, "tp"), P(None, "tp", "sp", None), P(None, "tp"))
    return jax.shard_map(
        local, mesh=mesh, in_specs=placed, out_specs=P("sp", "tp"), check_vma=False
    )
```
